32 devices in a mesh: fs: 8 (over z, y), tp: 4 (over x, core).
Axes of the slice: x: 2, y: 2, z: 4, core: 2. Of those that a mesh axis runs over, the one named last changes fastest.
Arguments:
- x_saved: bfloat16 [16384, 2048], P('fs'), may hold values from -6 to 6
- h_saved: bfloat16 [16384, 1024], P('fs', 'tp'), may hold values from -6 to 6
- key_cot: bfloat16 [16384, 1024], P('fs', 'tp'), may hold values from -6 to 6
- value_cot: bfloat16 [16384, 1024], P('fs', 'tp'), may hold values from -6 to 6
- out_cot: bfloat16 [16384, 2048], P('fs'), may hold values from -6 to 6
- w_key: float32 [2048, 1024], P('fs', 'tp'), may hold values from -0.125 to 0.125
- w_value: float32 [2048, 1024], P('fs', 'tp'), may hold values from -0.125 to 0.125
- w_out: float32 [1024, 2048], P('tp', 'fs'), may hold values from -0.1875 to 0.1875
- p_key: bfloat16 [2048, 256], P('fs'), may hold values from -1 to 1, as said below
- p_value: bfloat16 [2048, 256], P('fs'), may hold values from -1 to 1, as said below
- p_out: bfloat16 [2048, 256], P('fs'), may hold values from -1 to 1, as said below
- m_key: float32 [2, 256, 1024], P(None, 'fs', 'tp'), may hold values from -1.5 to 1.5, as said below
- m_value: float32 [2, 256, 1024], P(None, 'fs', 'tp'), may hold values from -1.5 to 1.5, as said below
- m_out: float32 [2, 256, 1024], P(None, 'fs', 'tp'), may hold values from -1.5 to 1.5, as said below
Outputs:
- step_key: float32 [2048, 1024], P('fs', 'tp')
- step_value: float32 [2048, 1024], P('fs', 'tp')
- step_out: float32 [1024, 2048], P('tp', 'fs')
- copy_key: bfloat16 [2048, 1024], P(None, 'tp')
- copy_value: bfloat16 [2048, 1024], P(None, 'tp')
- copy_out: bfloat16 [1024, 2048], P('tp')
- new_m_key: float32 [2, 256, 1024], P(None, 'fs', 'tp')
- new_m_value: float32 [2, 256, 1024], P(None, 'fs', 'tp')
- new_m_out: float32 [2, 256, 1024], P(None, 'fs', 'tp')
The draws below stay inside these ranges and needn't reach their ends.
Inputs may be any that keep to these rules, and one draw needn't show every extreme that they name: `p_key`: factor entries are real-valued, dense and of full rank. `p_value`: factor entries are real-valued, dense and of full rank. `p_out`: factor entries are real-valued, dense and of full rank. `m_key`: plane 1 (second moments) lies in 0.05 to 1. `m_value`: plane 1 (second moments) lies in 0.05 to 1. `m_out`: plane 1 (second moments) lies in 0.05 to 1.
All inputs are finite; a program needn't handle non-finite values.
Results may differ from the reference program's by a relative error of at most 0.0085.
Values may be sent and summed in bfloat16 or wider, within the bound.
A program may use at most 128 MiB of HBM per device.

```python
import math
import jax
import jax.numpy as jnp
from jax import lax

D = 2048
HW = 1024
RANK = 256
TOKENS = 16384


def factor_draw(key, member):
    key = jax.random.fold_in(key, member)
    key_base, key_cols = jax.random.split(key, 2)
    gaussian = jax.random.truncated_normal(key_base, -4.0, 4.0, (D, RANK), jnp.float32)
    columns = jnp.arange(RANK, dtype=jnp.float32)
    rising = 10.0 ** (columns / RANK) * jax.random.uniform(key_cols, (RANK,), jnp.float32, 0.7, 1.4)
    factor_values = gaussian * rising[None, :] * D ** (-0.5)
    return jnp.clip(factor_values, -1.0, 1.0).astype(jnp.bfloat16)


def moment_draw(key, member):
    key = jax.random.fold_in(key, member)
    key_one, key_two = jax.random.split(key)
    plane_one = 0.3 * jax.random.truncated_normal(key_one, -5.0, 5.0, (RANK, HW), jnp.float32)
    plane_two = jnp.exp(jax.random.uniform(key_two, (RANK, HW), jnp.float32, math.log(0.05), 0.0))
    return jnp.stack([plane_one, plane_two]).astype(jnp.float32)


def draw_p_key(key, part):
    return factor_draw(key, 11)


def draw_p_value(key, part):
    return factor_draw(key, 12)


def draw_p_out(key, part):
    return factor_draw(key, 13)


def draw_m_key(key, part):
    return moment_draw(key, 21)


def draw_m_value(key, part):
    return moment_draw(key, 22)


def draw_m_out(key, part):
    return moment_draw(key, 23)


def block_levels(rng, dims, pieces, smallest, top_value):
    def one(position, parts):
        draws = jax.random.uniform(jax.random.fold_in(jax.random.fold_in(rng, 6), position), (parts,), jnp.float32, smallest / len(pieces), top_value / len(pieces))
        return jnp.repeat(jnp.exp(draws), dims[position] // parts).reshape((-1,) + (1,) * (len(dims) - position - 1))

    loudness = one(*pieces[0])
    for cut in pieces[1:]:
        loudness = loudness * one(*cut)
    return loudness


def normal_values(key, extent, width, limit, cuts=(), kind=jnp.bfloat16):
    values = jax.random.normal(key, extent, jnp.float32) * width
    if len(cuts) > 0:
        values = block_levels(key, extent, cuts, -0.22, 0.18) * values
    return jnp.clip(values, min=-limit, max=limit).astype(kind)


def setup_inputs(seed: int = 0) -> dict:
    keys = jax.random.split(jax.random.key(seed), 15)
    x_saved = normal_values(keys[0], (TOKENS, D), 1.0, 6.0, ((0, 8),))
    h_saved = normal_values(keys[1], (TOKENS, HW), 1.0, 6.0, ((0, 8), (1, 4)))
    key_cot = normal_values(keys[2], (TOKENS, HW), 1.0, 6.0, ((0, 8), (1, 4)))
    value_cot = normal_values(keys[3], (TOKENS, HW), 1.0, 6.0, ((0, 8), (1, 4)))
    out_cot = normal_values(keys[4], (TOKENS, D), 1.0, 6.0, ((0, 8),))
    w_key = normal_values(keys[5], (D, HW), D ** -0.5, 0.125, ((0, 8), (1, 4)), jnp.float32)
    w_value = normal_values(keys[6], (D, HW), D ** -0.5, 0.125, ((0, 8), (1, 4)), jnp.float32)
    w_out = normal_values(keys[7], (HW, D), HW ** -0.5, 0.1875, ((0, 4), (1, 8)), jnp.float32)
    p_key = draw_p_key(jax.random.fold_in(keys[14], 71), 0)
    p_value = draw_p_value(jax.random.fold_in(keys[14], 71), 0)
    p_out = draw_p_out(jax.random.fold_in(keys[14], 71), 0)
    m_key = draw_m_key(jax.random.fold_in(keys[14], 71), 0)
    m_value = draw_m_value(jax.random.fold_in(keys[14], 71), 0)
    m_out = draw_m_out(jax.random.fold_in(keys[14], 71), 0)
    return dict(x_saved=x_saved, h_saved=h_saved, key_cot=key_cot, value_cot=value_cot, out_cot=out_cot, w_key=w_key, w_value=w_value, w_out=w_out, p_key=p_key, p_value=p_value, p_out=p_out, m_key=m_key, m_value=m_value, m_out=m_out)


beta_one = 0.9
beta_two = 0.9
learn_rate = 0.01

def exact_dot(left, right):
    return jnp.dot(left.astype(jnp.float32), right.astype(jnp.float32), precision=lax.Precision.HIGHEST)

def reference(x_saved, h_saved, key_cot, value_cot, out_cot, w_key, w_value, w_out, p_key, p_value, p_out, m_key, m_value, m_out):
    x_wide = x_saved.astype(jnp.float32).T
    grad_key = exact_dot(x_wide, key_cot)
    grad_value = exact_dot(x_wide, value_cot)
    grad_out_t = exact_dot(out_cot.astype(jnp.float32).T, h_saved)
    factors = (p_key, p_value, p_out)
    projected = [exact_dot(factors[0].astype(jnp.float32).T, grad_key), exact_dot(factors[1].astype(jnp.float32).T, grad_value), exact_dot(factors[2].astype(jnp.float32).T, grad_out_t)]
    total = jnp.sum(projected[0] * projected[0]) + jnp.sum(projected[1] * projected[1]) + jnp.sum(projected[2] * projected[2])
    norm_scale = jnp.sqrt(total / (3 * RANK * HW) + 1e-06)
    olds = (m_key, m_value, m_out)
    steps = []
    moments = []
    for member in range(3):
        normed = projected[member] / norm_scale
        moment_one = beta_one * olds[member][0] + (1 - beta_one) * normed
        moment_two = beta_two * olds[member][1] + (1 - beta_two) * normed * normed
        direction = (moment_one / jnp.sqrt(moment_two)).astype(jnp.bfloat16)
        steps.append(exact_dot(factors[member], direction))
        moments.append(jnp.stack([moment_one, moment_two]))
    step_key = steps[0]
    step_value = steps[1]
    step_out = steps[2].T
    copy_key = (w_key - learn_rate * step_key).astype(jnp.bfloat16)
    copy_value = (w_value - learn_rate * step_value).astype(jnp.bfloat16)
    copy_out = (w_out - learn_rate * step_out).astype(jnp.bfloat16)
    return (step_key, step_value, step_out, copy_key, copy_value, copy_out, moments[0], moments[1], moments[2])
```

```python
import functools

import jax
import jax.numpy as jnp
from jax import lax
from jax.experimental import pallas as pl
from jax.experimental.pallas import tpu as pltpu
from jax.sharding import PartitionSpec as P

beta_one = 0.9
beta_two = 0.9
learn_rate = 0.01
MESH = pl.DeviceIdType.MESH
f32 = jnp.float32
bf16 = jnp.bfloat16


def remote(src, dst, send_sem, recv_sem, target):
    return pltpu.make_async_remote_copy(
        src_ref=src, dst_ref=dst, send_sem=send_sem, recv_sem=recv_sem,
        device_id=target, device_id_type=MESH,
    )


class Gather:
    def __init__(self, view, send_sem, recv, place, span, order, sibling=None):
        self.view, self.send_sem, self.recv = view, send_sem, recv
        self.z, self.b = place
        self.span, self.order, self.sibling = span, order, sibling
        self.sends = []

    def index(self, z, b):
        return z * 2 + b

    def send(self, cond, z, b, to):
        j = self.index(z, b)

        def copy():
            return remote(self.view(j), self.view(j), self.send_sem, self.recv.at[j], {"fs": to})

        if cond is None:
            copy().start()
        else:
            pl.when(cond)(lambda: copy().start())
        self.sends.append((cond, copy))

    def to_sibling(self, cond, z, b):
        if self.sibling is None:
            return
        target, recv = self.sibling
        j = self.index(z, b)

        def copy():
            return remote(self.view(j), self.view(j), self.send_sem, recv.at[j], {"tp": target})

        if cond is None:
            copy().start()
        else:
            pl.when(cond)(lambda: copy().start())
        self.sends.append((cond, copy))

    def arrive(self, cond, z, b):
        j = self.index(z, b)

        def wait():
            remote(self.view(j), self.view(j), self.send_sem, self.recv.at[j], {"fs": j}).wait_recv()

        if cond is None:
            wait()
        else:
            pl.when(cond)(wait)

    def up_down(self, b):
        z = self.z
        self.send(z < self.span - 1, z, b, self.index(z + 1, self.b))
        self.send(z > 0, z, b, self.index(z - 1, self.b))

    def begin(self):
        z, b = self.z, self.b
        pair = self.index(z, 1 - b)
        if self.order == "line":
            self.up_down(b)
            self.send(None, z, b, pair)
        else:
            self.send(None, z, b, pair)
            self.up_down(b)
        self.to_sibling(None, z, b)

    def cross(self):
        if self.order == "pair":
            self.arrive(None, self.z, 1 - self.b)
            self.up_down(1 - self.b)
            self.to_sibling(None, self.z, 1 - self.b)

    def step(self, s):
        z, b, span = self.z, self.b, self.span
        for b_from in (b,) if self.order == "line" else (b, 1 - b):
            for sign in (1, -1):
                zf = z - sign * s
                have = (zf >= 0) if sign == 1 else (zf < span)
                more = (z < span - 1) if sign == 1 else (z > 0)
                self.arrive(have, zf, b_from)
                self.send(jnp.logical_and(have, more), zf, b_from, self.index(z + sign, b))
                if self.order == "line":
                    self.send(have, zf, b, self.index(z, 1 - b))
                self.to_sibling(have, zf, b_from)

    def cross_end(self):
        if self.order == "line":
            for zf in range(self.span):
                self.arrive(None, zf, 1 - self.b)
                self.to_sibling(None, zf, 1 - self.b)

    def sibling_end(self, view):
        target, recv = self.sibling
        for j in range(2 * self.span):
            remote(view(j), view(j), self.send_sem, recv.at[j], {"tp": target}).wait_recv()

    def finish(self):
        for cond, copy in self.sends:
            if cond is None:
                copy().wait_send()
            else:
                pl.when(cond)(lambda copy=copy: copy().wait_send())


def kernel(
    n, t, chunk, entries,
    x_hbm, y_hbm, k_hbm, v_hbm, h_hbm, p_in, w_in, mk_in, mv_in, mo_in,
    p_out, w_out, d_out, nk_out, nv_out, no_out,
    x_buf, y_buf, c_buf, ct_buf, g_buf, part_out, part_in, sq_tp, sq_fs, sq_sum,
    load_sem, own_sem, g_send, pa_recv, pb_recv, pa_sib, pb_sib, wa_recv, wb_recv,
    r_send, r_recv, st_send, st_recv, sf_send, sf_recv, d_send, d_recv,
):
    me, tp = lax.axis_index("fs"), lax.axis_index("tp")
    place = (me // 2, me % 2)
    span = n // 2
    half = tp % 2
    sibling = tp + 1 - 2 * half
    tokens, width = x_hbm.shape
    columns = k_hbm.shape[1]
    rows = part_in.shape[1]
    n_chunks = width // chunk

    loads = [
        pltpu.make_async_copy(src, c_buf.at[:, pl.ds(i * columns, columns)], load_sem.at[i])
        for i, src in enumerate((k_hbm, v_hbm, h_hbm))
    ]
    x_loads = [
        pltpu.make_async_copy(src.at[:, pl.ds(c * chunk, chunk)], dst.at[c], load_sem.at[3 + o * n_chunks + c])
        for o, (src, dst) in enumerate(((x_hbm, x_buf), (y_hbm, y_buf)))
        for c in range(n_chunks)
    ]
    own_p = pltpu.make_async_copy(p_in, p_out.at[:, pl.ds(2 * me, 2)], own_sem.at[0])
    own_w = pltpu.make_async_copy(w_in, w_out.at[:, me], own_sem.at[1])
    own_p.start()
    own_w.start()
    for load in loads + x_loads:
        load.start()

    barrier = pltpu.get_barrier_semaphore()
    for k in range(1, n):
        pl.semaphore_signal(barrier, inc=1, device_id={"fs": lax.rem(me + k, n)}, device_id_type=MESH)
    for k in range(1, t):
        pl.semaphore_signal(barrier, inc=1, device_id={"tp": lax.rem(tp + k, t)}, device_id_type=MESH)
    pl.semaphore_wait(barrier, n + t - 2)

    def p_view(low, high, side):
        return lambda j: p_out.at[low:high, 2 * j + side]

    own_p.wait()
    own_w.wait()
    pa = Gather(p_view(0, 2, half), g_send.at[0], pa_recv, place, span, "line", (sibling, pa_sib))
    pb = Gather(p_view(2, 3, half), g_send.at[1], pb_recv, place, span, "pair", (sibling, pb_sib))
    wa = Gather(lambda j: w_out.at[0:2, j], g_send.at[2], wa_recv, place, span, "line")
    wb = Gather(lambda j: w_out.at[2:3, j], g_send.at[3], wb_recv, place, span, "pair")
    sib_a, pa.sibling = pa.sibling, None
    sib_b, pb.sibling = pb.sibling, None
    pb.begin()
    pa.begin()
    pa.sibling, pb.sibling = sib_a, sib_b

    for load in loads:
        load.wait()
    ct_buf[...] = c_buf[...].T

    def grads(o, c):
        x_loads[o * n_chunks + c].wait()
        lo, hi = (0, 2 * columns) if o == 0 else (2 * columns, 3 * columns)
        g_buf[lo:hi, c * chunk:(c + 1) * chunk] = jnp.dot(
            ct_buf[lo:hi, :], (x_buf, y_buf)[o][c], preferred_element_type=f32
        ).astype(bf16)

    work = [(o, c) for o in range(2) for c in range(n_chunks)]
    per = -(-len(work) // (span - 1 + 1))
    todo = list(work)

    def some():
        for _ in range(per):
            if todo:
                grads(*todo.pop(0))

    some()
    pb.cross()
    for s in range(1, span):
        pa.step(s)
        pb.step(s)
        some()
    while todo:
        grads(*todo.pop(0))
    pa.cross_end()
    wb.begin()
    wa.begin()

    def sib_end(gather, low, high):
        target, recv = gather.sibling
        view = p_view(low, high, 1 - half)
        for j in range(n):
            @pl.when(me != j)
            def _():
                remote(view(j), view(j), gather.send_sem, recv.at[j], {"tp": target}).wait_recv()

    sib_end(pa, 0, 2)
    sib_end(pb, 2, 3)

    for m in range(3):
        full = p_out[m].reshape(width, p_out.shape[3])
        proj = jnp.dot(g_buf[m * columns:(m + 1) * columns, :], full, preferred_element_type=f32)
        part_out[:, :, m * columns:(m + 1) * columns] = proj.T.astype(bf16).reshape(n, rows, columns)

    part_copies = []
    for k in range(1, n):
        to = lax.rem(me + k, n)
        copy = remote(part_out.at[to], part_in.at[k], r_send.at[k], r_recv.at[k], {"fs": to})
        copy.start()
        part_copies.append(copy)
    wb.cross()
    total = part_out[me].astype(f32)
    for copy in part_copies:
        copy.wait_recv()
    for k in range(1, n):
        total = total + part_in[k].astype(f32)

    squares = jnp.sum(total * total, axis=0, keepdims=True)
    square = jnp.sum(squares, axis=1, keepdims=True)
    sq_tp[tp] = jnp.broadcast_to(square, (8, 128))
    tp_copies = []
    for k in range(1, t):
        to = lax.rem(tp + k, t)
        copy = remote(sq_tp.at[tp], sq_tp.at[tp], st_send.at[k], st_recv.at[k], {"tp": to})
        copy.start()
        tp_copies.append(copy)
    for copy in tp_copies:
        copy.wait_recv()
    sum_tp = sq_tp[0]
    for k in range(1, t):
        sum_tp = sum_tp + sq_tp[k]
    sq_fs[me] = sum_tp
    fs_copies = []
    for k in range(1, n):
        to = lax.rem(me + k, n)
        copy = remote(sq_fs.at[me], sq_fs.at[me], sf_send.at[k], sf_recv.at[k], {"fs": to})
        copy.start()
        fs_copies.append(copy)
    for copy in fs_copies:
        copy.wait_recv()
    sum_fs = sq_fs[0]
    for k in range(1, n):
        sum_fs = sum_fs + sq_fs[k]
    scale = 1.0 / jnp.sqrt(sum_fs[0:1, 0:1] / entries + 1e-06)
    normed = total * scale

    for m, (old, new) in enumerate(((mk_in, nk_out), (mv_in, nv_out), (mo_in, no_out))):
        q = normed[:, m * columns:(m + 1) * columns]
        one = beta_one * old[0] + (1 - beta_one) * q
        two = beta_two * old[1] + (1 - beta_two) * q * q
        new[0] = one
        new[1] = two
        d_out[me, :, m * columns:(m + 1) * columns] = (one / jnp.sqrt(two)).astype(bf16)
    d_copies = []
    for k in range(1, n):
        to = lax.rem(me + k, n)
        copy = remote(d_out.at[me], d_out.at[me], d_send.at[k], d_recv.at[k], {"fs": to})
        copy.start()
        d_copies.append(copy)
    for s in range(1, span):
        wa.step(s)
        wb.step(s)
    wa.cross_end()
    for copy in d_copies:
        copy.wait_recv()
    for copy in part_copies + tp_copies + fs_copies + d_copies:
        copy.wait_send()
    for gather in (pa, pb, wa, wb):
        gather.finish()


def body(
    x_saved, h_saved, key_cot, value_cot, out_cot, w_key, w_value, w_out,
    p_key, p_value, p_out, m_key, m_value, m_out,
):
    n, t = lax.axis_size("fs"), lax.axis_size("tp")
    tokens, width = x_saved.shape
    columns = key_cot.shape[1]
    local, rank = p_key.shape
    rows = rank // n
    chunk = min(512, width)
    n_chunks = width // chunk
    p_stack = jnp.stack([p_key, p_value, p_out]).reshape(3, 2, local // 2, rank)
    w_stack = jnp.stack([w_key.astype(bf16), w_value.astype(bf16), w_out.T.astype(bf16)])
    entries = 3 * rank * columns * t
    any_spec = pl.BlockSpec(memory_space=pl.ANY)
    vmem = pl.BlockSpec(memory_space=pltpu.VMEM)
    dma = pltpu.SemaphoreType.DMA
    moment = jax.ShapeDtypeStruct(m_key.shape, f32)
    p_full, w_full, d_full, new_k, new_v, new_o = pl.pallas_call(
        functools.partial(kernel, n, t, chunk, entries),
        out_shape=(
            jax.ShapeDtypeStruct((3, 2 * n, local // 2, rank), bf16),
            jax.ShapeDtypeStruct((3, n, local, columns), bf16),
            jax.ShapeDtypeStruct((n, rows, 3 * columns), bf16),
            moment, moment, moment,
        ),
        in_specs=[any_spec] * 5 + [vmem] * 5,
        out_specs=(vmem,) * 6,
        scratch_shapes=[
            pltpu.VMEM((n_chunks, tokens, chunk), bf16),
            pltpu.VMEM((n_chunks, tokens, chunk), bf16),
            pltpu.VMEM((tokens, 3 * columns), bf16),
            pltpu.VMEM((3 * columns, tokens), bf16),
            pltpu.VMEM((3 * columns, width), bf16),
            pltpu.VMEM((n, rows, 3 * columns), bf16),
            pltpu.VMEM((n, rows, 3 * columns), bf16),
            pltpu.VMEM((t, 8, 128), f32),
            pltpu.VMEM((n, 8, 128), f32),
            pltpu.VMEM((8, 128), f32),
            dma((3 + 2 * n_chunks,)),
            dma((2,)),
            dma((4,)),
            dma((n,)), dma((n,)), dma((n,)), dma((n,)), dma((n,)), dma((n,)),
            dma((n,)), dma((n,)), dma((t,)), dma((t,)),
            dma((n,)), dma((n,)), dma((n,)), dma((n,)),
        ],
        compiler_params=pltpu.CompilerParams(
            collective_id=0, has_side_effects=True, vmem_limit_bytes=60 * 1024 * 1024
        ),
        name="fused_update",
    )(x_saved, out_cot, key_cot, value_cot, h_saved, p_stack, w_stack, m_key, m_value, m_out)

    direction = d_full.reshape(rank, 3 * columns)
    factors = p_full.reshape(3, width, rank)
    weights = w_full.reshape(3, width, columns)
    parts = [direction[:, m * columns:(m + 1) * columns] for m in range(3)]
    dot = functools.partial(jnp.dot, preferred_element_type=f32)
    step_key, step_value = dot(p_key, parts[0]), dot(p_value, parts[1])
    step_out = dot(parts[2].T, p_out.T)
    copies = [
        (weights[m].astype(f32) - learn_rate * dot(factors[m], parts[m])).astype(bf16)
        for m in range(2)
    ]
    copy_out = (weights[2].T.astype(f32) - learn_rate * dot(parts[2].T, factors[2].T)).astype(bf16)
    return (step_key, step_value, step_out, copies[0], copies[1], copy_out, new_k, new_v, new_o)


def solution(mesh):
    in_specs = (
        P("fs", None), P("fs", "tp"), P("fs", "tp"), P("fs", "tp"), P("fs", None),
        P("fs", "tp"), P("fs", "tp"), P("tp", "fs"),
        P("fs", None), P("fs", None), P("fs", None),
        P(None, "fs", "tp"), P(None, "fs", "tp"), P(None, "fs", "tp"),
    )
    out_specs = (
        P("fs", "tp"), P("fs", "tp"), P("tp", "fs"),
        P(None, "tp"), P(None, "tp"), P("tp", None),
        P(None, "fs", "tp"), P(None, "fs", "tp"), P(None, "fs", "tp"),
    )
    return jax.shard_map(body, mesh=mesh, in_specs=in_specs, out_specs=out_specs, check_vma=False)
```

```python
import functools

import jax
import jax.numpy as jnp
from jax import lax
from jax.experimental import pallas as pl
from jax.experimental.pallas import tpu as pltpu
from jax.sharding import PartitionSpec as P

beta_one = 0.9
beta_two = 0.9
learn_rate = 0.01
MESH = pl.DeviceIdType.MESH
f32 = jnp.float32
bf16 = jnp.bfloat16


def remote(src, dst, send_sem, recv_sem, target):
    return pltpu.make_async_remote_copy(
        src_ref=src, dst_ref=dst, send_sem=send_sem, recv_sem=recv_sem,
        device_id=target, device_id_type=MESH,
    )


class Gather:
    def __init__(self, view, send_sem, recv, place, span, order, sibling=None):
        self.view, self.send_sem, self.recv = view, send_sem, recv
        self.z, self.b = place
        self.span, self.order, self.sibling = span, order, sibling
        self.sends = []

    def index(self, z, b):
        return z * 2 + b

    def send(self, cond, z, b, to):
        j = self.index(z, b)

        def copy():
            return remote(self.view(j), self.view(j), self.send_sem, self.recv.at[j], {"fs": to})

        if cond is None:
            copy().start()
        else:
            pl.when(cond)(lambda: copy().start())
        self.sends.append((cond, copy))

    def to_sibling(self, cond, z, b):
        if self.sibling is None:
            return
        target, recv = self.sibling
        j = self.index(z, b)

        def copy():
            return remote(self.view(j), self.view(j), self.send_sem, recv.at[j], {"tp": target})

        if cond is None:
            copy().start()
        else:
            pl.when(cond)(lambda: copy().start())
        self.sends.append((cond, copy))

    def arrive(self, cond, z, b):
        j = self.index(z, b)

        def wait():
            remote(self.view(j), self.view(j), self.send_sem, self.recv.at[j], {"fs": j}).wait_recv()

        if cond is None:
            wait()
        else:
            pl.when(cond)(wait)

    def up_down(self, b):
        z = self.z
        self.send(z < self.span - 1, z, b, self.index(z + 1, self.b))
        self.send(z > 0, z, b, self.index(z - 1, self.b))

    def begin(self):
        z, b = self.z, self.b
        pair = self.index(z, 1 - b)
        if self.order == "line":
            self.up_down(b)
            self.send(None, z, b, pair)
        else:
            self.send(None, z, b, pair)
            self.up_down(b)
        self.to_sibling(None, z, b)

    def cross(self):
        if self.order == "pair":
            self.arrive(None, self.z, 1 - self.b)
            self.up_down(1 - self.b)
            self.to_sibling(None, self.z, 1 - self.b)

    def step(self, s):
        z, b, span = self.z, self.b, self.span
        for b_from in (b,) if self.order == "line" else (b, 1 - b):
            for sign in (1, -1):
                zf = z - sign * s
                have = (zf >= 0) if sign == 1 else (zf < span)
                more = (z < span - 1) if sign == 1 else (z > 0)
                self.arrive(have, zf, b_from)
                self.send(jnp.logical_and(have, more), zf, b_from, self.index(z + sign, b))
                if self.order == "line":
                    self.send(have, zf, b, self.index(z, 1 - b))
                self.to_sibling(have, zf, b_from)

    def cross_end(self):
        if self.order == "line":
            for zf in range(self.span):
                self.arrive(None, zf, 1 - self.b)
                self.to_sibling(None, zf, 1 - self.b)

    def sibling_end(self, view):
        target, recv = self.sibling
        for j in range(2 * self.span):
            remote(view(j), view(j), self.send_sem, recv.at[j], {"tp": target}).wait_recv()

    def finish(self):
        for cond, copy in self.sends:
            if cond is None:
                copy().wait_send()
            else:
                pl.when(cond)(lambda copy=copy: copy().wait_send())


def moments(old, q):
    return (
        beta_one * old[0] + (1 - beta_one) * q,
        beta_two * old[1] + (1 - beta_two) * q * q,
    )


def finish_kernel(
    columns, p_ref, w_ref, d_ref, q_ref, pk_ref, pv_ref, po_ref, mk_ref, mv_ref, mo_ref,
    sk_ref, sv_ref, so_ref, ck_ref, cv_ref, co_ref, nk_ref, nv_ref, no_ref,
):
    def step(factor, m):
        return jnp.dot(factor, d_ref[:, m * columns:(m + 1) * columns], preferred_element_type=f32)

    def fresh(m):
        return (w_ref[m].astype(f32) - learn_rate * step(p_ref[m], m)).astype(bf16)

    ck_ref[...] = fresh(0)
    cv_ref[...] = fresh(1)
    co_ref[...] = fresh(2).T

    @pl.when(pl.program_id(0) == 0)
    def _():
        sk_ref[...] = step(pk_ref[...], 0)
        sv_ref[...] = step(pv_ref[...], 1)
        so_ref[...] = step(po_ref[...], 2).T
        for m, (old, new) in enumerate(((mk_ref, nk_ref), (mv_ref, nv_ref), (mo_ref, no_ref))):
            new[0], new[1] = moments(old, q_ref[:, m * columns:(m + 1) * columns])


def kernel(
    n, t, chunk, entries,
    x_hbm, y_hbm, k_hbm, v_hbm, h_hbm, pk_hbm, pv_hbm, po_hbm, wk_hbm, wv_hbm, wo_hbm, mk_in, mv_in, mo_in,
    p_out, w_out, d_out, q_out,
    x_buf, y_buf, c_buf, ct_buf, g_buf, wk_buf, wv_buf, wo_buf, part_out, part_in, sq_tp, sq_fs,
    load_sem, own_sem, g_send, p_recv, p_sib, w_recv,
    r_send, r_recv, st_send, st_recv, sf_send, sf_recv, d_send, d_recv,
):
    me, tp = lax.axis_index("fs"), lax.axis_index("tp")
    place = (me // 2, me % 2)
    span = n // 2
    half = tp % 2
    sibling = tp + 1 - 2 * half
    tokens, width = x_hbm.shape
    columns = k_hbm.shape[1]
    rows = part_in.shape[1]
    n_chunks = width // chunk

    loads = [
        pltpu.make_async_copy(src, c_buf.at[:, pl.ds(i * columns, columns)], load_sem.at[i])
        for i, src in enumerate((k_hbm, v_hbm, h_hbm))
    ]
    x_loads = [
        pltpu.make_async_copy(src.at[:, pl.ds(c * chunk, chunk)], dst.at[c], load_sem.at[3 + o * n_chunks + c])
        for o, (src, dst) in enumerate(((x_hbm, x_buf), (y_hbm, y_buf)))
        for c in range(n_chunks)
    ]
    own_p = [
        pltpu.make_async_copy(src, p_out.at[m, pl.ds(2 * me, 2)], own_sem.at[m])
        for m, src in enumerate((pk_hbm, pv_hbm, po_hbm))
    ]
    own_w = [
        pltpu.make_async_copy(src, dst, own_sem.at[3 + m])
        for m, (src, dst) in enumerate(((wk_hbm, wk_buf), (wv_hbm, wv_buf), (wo_hbm, wo_buf)))
    ]
    for load in own_p:
        load.start()
    for load in loads + x_loads + own_w:
        load.start()

    barrier = pltpu.get_barrier_semaphore()
    for k in range(1, n):
        pl.semaphore_signal(barrier, inc=1, device_id={"fs": lax.rem(me + k, n)}, device_id_type=MESH)
    for k in range(1, t):
        pl.semaphore_signal(barrier, inc=1, device_id={"tp": lax.rem(tp + k, t)}, device_id_type=MESH)
    pl.semaphore_wait(barrier, n + t - 2)

    def p_view(m, side):
        return lambda j: p_out.at[m, 2 * j + side]

    def w_view(m):
        return lambda j: w_out.at[m, j]

    for load in own_p:
        load.wait()
    orders = ("line", "line", "pair")
    ps = [
        Gather(p_view(m, half), g_send.at[m], p_recv.at[m], place, span, orders[m], (sibling, p_sib.at[m]))
        for m in range(3)
    ]
    ws = [Gather(w_view(m), g_send.at[3 + m], w_recv.at[m], place, span, orders[m]) for m in range(3)]
    for m in (2, 0, 1):
        to, ps[m].sibling = ps[m].sibling, None
        ps[m].begin()
        ps[m].sibling = to

    for load in loads:
        load.wait()
    ct_buf[...] = c_buf[...].T

    def grads(o, c):
        x_loads[o * n_chunks + c].wait()
        lo, hi = (0, 2 * columns) if o == 0 else (2 * columns, 3 * columns)
        g_buf[lo:hi, c * chunk:(c + 1) * chunk] = jnp.dot(
            ct_buf[lo:hi, :], (x_buf, y_buf)[o][c], preferred_element_type=f32
        ).astype(bf16)

    work = [(o, c) for o in range(2) for c in range(n_chunks)]
    per = -(-len(work) // (span - 1 + 1))
    todo = list(work)

    def some():
        for _ in range(per):
            if todo:
                grads(*todo.pop(0))

    some()
    ps[2].cross()
    for s in range(1, span):
        for m in (0, 1, 2):
            ps[m].step(s)
        if s == 1:
            for load in own_w:
                load.wait()
            w_out[0, me] = wk_buf[...].astype(bf16)
            w_out[1, me] = wv_buf[...].astype(bf16)
            w_out[2, me] = wo_buf[...].T.astype(bf16)
        some()
    while todo:
        grads(*todo.pop(0))
    for m in (2, 0, 1):
        ws[m].begin()
    for m in (0, 1):
        ps[m].cross_end()
    for m in range(3):
        target, recv = ps[m].sibling
        view = p_view(m, 1 - half)
        for j in range(n):
            @pl.when(me != j)
            def _(view=view, recv=recv, m=m, target=target, j=j):
                remote(view(j), view(j), ps[m].send_sem, recv.at[j], {"tp": target}).wait_recv()

    for m in range(3):
        full = p_out[m].reshape(width, p_out.shape[3])
        proj = jnp.dot(g_buf[m * columns:(m + 1) * columns, :], full, preferred_element_type=f32)
        part_out[:, :, m * columns:(m + 1) * columns] = proj.T.astype(bf16).reshape(n, rows, columns)

    part_copies = []
    for k in range(1, n):
        to = lax.rem(me + k, n)
        copy = remote(part_out.at[to], part_in.at[k], r_send.at[k], r_recv.at[k], {"fs": to})
        copy.start()
        part_copies.append(copy)
    ws[2].cross()
    for s in range(1, min(2, span)):
        for m in (0, 1, 2):
            ws[m].step(s)
    total = part_out[me].astype(f32)
    for copy in part_copies:
        copy.wait_recv()
    for k in range(1, n):
        total = total + part_in[k].astype(f32)

    squares = jnp.sum(total * total, axis=0, keepdims=True)
    square = jnp.sum(squares, axis=1, keepdims=True)
    sq_tp[tp] = jnp.broadcast_to(square, (8, 128))
    tp_copies = []
    for k in range(1, t):
        to = lax.rem(tp + k, t)
        copy = remote(sq_tp.at[tp], sq_tp.at[tp], st_send.at[k], st_recv.at[k], {"tp": to})
        copy.start()
        tp_copies.append(copy)
    for copy in tp_copies:
        copy.wait_recv()
    sum_tp = sq_tp[0]
    for k in range(1, t):
        sum_tp = sum_tp + sq_tp[k]
    sq_fs[me] = sum_tp
    fs_copies = []
    for k in range(1, n):
        to = lax.rem(me + k, n)
        copy = remote(sq_fs.at[me], sq_fs.at[me], sf_send.at[k], sf_recv.at[k], {"fs": to})
        copy.start()
        fs_copies.append(copy)
    for s in range(2, min(3, span)):
        for m in (0, 1):
            ws[m].step(s)
    for copy in fs_copies:
        copy.wait_recv()
    sum_fs = sq_fs[0]
    for k in range(1, n):
        sum_fs = sum_fs + sq_fs[k]
    scale = 1.0 / jnp.sqrt(sum_fs[0:1, 0:1] / entries + 1e-06)
    normed = total * scale

    q_out[...] = normed
    for m, old in enumerate((mk_in, mv_in, mo_in)):
        one, two = moments(old, normed[:, m * columns:(m + 1) * columns])
        d_out[me, :, m * columns:(m + 1) * columns] = (one / jnp.sqrt(two)).astype(bf16)
    d_copies = []
    for k in range(1, n):
        to = lax.rem(me + k, n)
        copy = remote(d_out.at[me], d_out.at[me], d_send.at[k], d_recv.at[k], {"fs": to})
        copy.start()
        d_copies.append(copy)
    for s in range(2, min(3, span)):
        for m in (2,):
            ws[m].step(s)
    for s in range(3, span):
        for m in (0, 1, 2):
            ws[m].step(s)
    for m in (0, 1):
        ws[m].cross_end()
    for copy in d_copies:
        copy.wait_recv()
    for copy in part_copies + tp_copies + fs_copies + d_copies:
        copy.wait_send()
    for gather in ps + ws:
        gather.finish()


def body(
    x_saved, h_saved, key_cot, value_cot, out_cot, w_key, w_value, w_out,
    p_key, p_value, p_out, m_key, m_value, m_out,
):
    n, t = lax.axis_size("fs"), lax.axis_size("tp")
    tokens, width = x_saved.shape
    columns = key_cot.shape[1]
    local, rank = p_key.shape
    rows = rank // n
    chunk = min(512, width)
    n_chunks = width // chunk
    halves = [p.reshape(2, local // 2, rank) for p in (p_key, p_value, p_out)]
    entries = 3 * rank * columns * t
    any_spec = pl.BlockSpec(memory_space=pl.ANY)
    vmem = pl.BlockSpec(memory_space=pltpu.VMEM)
    dma = pltpu.SemaphoreType.DMA
    shape = jax.ShapeDtypeStruct
    p_full, w_full, d_full, normed = pl.pallas_call(
        functools.partial(kernel, n, t, chunk, entries),
        out_shape=(
            shape((3, 2 * n, local // 2, rank), bf16),
            shape((3, n, local, columns), bf16),
            shape((n, rows, 3 * columns), bf16),
            shape((rows, 3 * columns), f32),
        ),
        in_specs=[any_spec] * 11 + [vmem] * 3,
        out_specs=(vmem,) * 4,
        scratch_shapes=[
            pltpu.VMEM((n_chunks, tokens, chunk), bf16),
            pltpu.VMEM((n_chunks, tokens, chunk), bf16),
            pltpu.VMEM((tokens, 3 * columns), bf16),
            pltpu.VMEM((3 * columns, tokens), bf16),
            pltpu.VMEM((3 * columns, width), bf16),
            pltpu.VMEM((local, columns), f32),
            pltpu.VMEM((local, columns), f32),
            pltpu.VMEM((columns, local), f32),
            pltpu.VMEM((n, rows, 3 * columns), bf16),
            pltpu.VMEM((n, rows, 3 * columns), bf16),
            pltpu.VMEM((t, 8, 128), f32),
            pltpu.VMEM((n, 8, 128), f32),
            dma((3 + 2 * n_chunks,)),
            dma((6,)),
            dma((6,)),
            dma((3, n)), dma((3, n)), dma((3, n)),
            dma((n,)), dma((n,)), dma((t,)), dma((t,)),
            dma((n,)), dma((n,)), dma((n,)), dma((n,)),
        ],
        compiler_params=pltpu.CompilerParams(
            collective_id=0, has_side_effects=True, vmem_limit_bytes=60 * 1024 * 1024
        ),
        name="fused_update",
    )(
        x_saved, out_cot, key_cot, value_cot, h_saved, *halves,
        w_key, w_value, w_out, m_key, m_value, m_out,
    )

    block = min(512, width)
    whole = lambda *dims: pl.BlockSpec(dims, lambda i: (0,) * len(dims))
    moment = whole(*m_key.shape)
    factor = whole(local, rank)
    return pl.pallas_call(
        functools.partial(finish_kernel, columns),
        grid=(width // block,),
        out_shape=(
            shape((local, columns), f32), shape((local, columns), f32), shape((columns, local), f32),
            shape((width, columns), bf16), shape((width, columns), bf16), shape((columns, width), bf16),
            shape(m_key.shape, f32), shape(m_key.shape, f32), shape(m_key.shape, f32),
        ),
        in_specs=[
            pl.BlockSpec((3, block, rank), lambda i: (0, i, 0)),
            pl.BlockSpec((3, block, columns), lambda i: (0, i, 0)),
            whole(rank, 3 * columns), whole(rows, 3 * columns),
            factor, factor, factor, moment, moment, moment,
        ],
        out_specs=(
            whole(local, columns), whole(local, columns), whole(columns, local),
            pl.BlockSpec((block, columns), lambda i: (i, 0)),
            pl.BlockSpec((block, columns), lambda i: (i, 0)),
            pl.BlockSpec((columns, block), lambda i: (0, i)),
            moment, moment, moment,
        ),
        compiler_params=pltpu.CompilerParams(dimension_semantics=("arbitrary",)),
        name="finish",
    )(
        p_full.reshape(3, width, rank), w_full.reshape(3, width, columns),
        d_full.reshape(rank, 3 * columns), normed,
        p_key, p_value, p_out, m_key, m_value, m_out,
    )


def solution(mesh):
    in_specs = (
        P("fs", None), P("fs", "tp"), P("fs", "tp"), P("fs", "tp"), P("fs", None),
        P("fs", "tp"), P("fs", "tp"), P("tp", "fs"),
        P("fs", None), P("fs", None), P("fs", None),
        P(None, "fs", "tp"), P(None, "fs", "tp"), P(None, "fs", "tp"),
    )
    out_specs = (
        P("fs", "tp"), P("fs", "tp"), P("tp", "fs"),
        P(None, "tp"), P(None, "tp"), P("tp", None),
        P(None, "fs", "tp"), P(None, "fs", "tp"), P(None, "fs", "tp"),
    )
    return jax.shard_map(body, mesh=mesh, in_specs=in_specs, out_specs=out_specs, check_vma=False)
```
